32 devices in a mesh: sp: 4 (over y, x), tp: 8 (over z, core).
Axes of the slice: x: 2, y: 2, z: 4, core: 2. Of those that a mesh axis runs over, the one named last changes fastest.
Arguments:
- tokens: bfloat16 [8192, 2048], P('sp', 'tp'), may hold values from -6 to 6
- norm_gain: float32 [2048], replicated, may hold values from 0.1 to 1.9
- w_key: bfloat16 [2048, 1024], P(None, 'tp'), may hold values from -0.125 to 0.125
- w_decay: bfloat16 [2048, 1024], P(None, 'tp'), may hold values from -0.125 to 0.125
- w_value: bfloat16 [2048, 512], replicated, may hold values from -0.125 to 0.125
- decay_bias: float32 [1024], P('tp'), may hold values from 0 to 8.5
- gate_drift: float32 [8192], P('sp'), may hold values from -1 to 1
- queries: bfloat16 [1024], P('tp'), may hold values from -6 to 6
- out_gain: float32 [4, 512], P(None, 'sp'), may hold values from 0.1 to 1.9
Outputs:
- state_cache: bfloat16 [1024, 512], P('tp', 'sp')
- first_read: float32 [4, 512], P(None, 'sp')
The draws below stay inside these ranges and needn't reach their ends.
All inputs are finite; a program needn't handle non-finite values.
Results may differ from the reference program's by a relative error of at most 0.009.
Values may be sent and summed in bfloat16 or wider, within the bound.
A program may use at most 128 MiB of HBM per device.

```python
import jax
import jax.numpy as jnp
from jax import lax

D = 2048
QUERY_KEY_HEADS = 4
KEY_CHANNELS = 256
VALUE_CHANNELS = 512
SPAN = 2048
BLOCK = 128
LEN = 8192
N_SP = 4


def draw_decay_bias(key, part):
    first, second, third = jax.random.split(key, 3)
    count = QUERY_KEY_HEADS * KEY_CHANNELS
    slow = jax.random.uniform(first, (count,), jnp.float32) < 0.5
    slow_value = jnp.log(LEN / 12.0) + jax.random.uniform(second, (count,), jnp.float32, -0.5, 0.5)
    slow_value = jnp.clip(slow_value, 0.0, 8.4)
    fast_value = jax.random.uniform(third, (count,), jnp.float32, 0.0, 1.5)
    return jnp.where(slow, slow_value, fast_value).astype(jnp.float32)


def draw_gate_drift(key, part):
    first, second = jax.random.split(key, 2)
    groups = LEN // BLOCK
    values = jax.random.uniform(second, (groups,), jnp.float32, -1.0, 1.0)
    return jnp.repeat(values, BLOCK).astype(jnp.float32)


def level_of(key, shape, pieces, least, top_value):
    gain = 1.0
    for axis_at, shards_of in pieces:
        draws = jax.random.uniform(jax.random.fold_in(jax.random.fold_in(key, 6), axis_at), (shards_of,), jnp.float32, least / len(pieces), top_value / len(pieces))
        gain = gain * jnp.repeat(jnp.exp(draws), shape[axis_at] // shards_of).reshape((-1,) + (1,) * (len(shape) - 1 - axis_at))
    return gain


def scatter_about(rng, dims, spread, bound, pieces=(), kind=jnp.bfloat16):
    loudness = level_of(rng, dims, pieces, -0.22, 0.18) if pieces else 1.0
    entries = jax.random.normal(rng, dims, jnp.float32) * spread * loudness
    return jnp.minimum(jnp.maximum(entries, -bound), bound).astype(kind)


def setup_inputs(seed: int = 0) -> dict:
    key_of = jax.random.split(jax.random.key(seed), 10)
    return {
        "tokens": scatter_about(key_of[0], (LEN, D), 1.0, 6.0, ((0, 4), (1, 8))),
        "norm_gain": jnp.clip(1.0 + 0.18 * jax.random.normal(key_of[1], (D,), jnp.float32), 0.1, 1.9),
        "w_key": scatter_about(key_of[2], (D, QUERY_KEY_HEADS * KEY_CHANNELS), D ** -0.5, 0.125, ((1, 8),)),
        "w_decay": scatter_about(key_of[3], (D, QUERY_KEY_HEADS * KEY_CHANNELS), D ** -0.5, 0.125, ((1, 8),)),
        "w_value": scatter_about(key_of[4], (D, VALUE_CHANNELS), D ** -0.5, 0.125),
        "decay_bias": draw_decay_bias(jax.random.fold_in(key_of[9], 71), 0),
        "gate_drift": draw_gate_drift(jax.random.fold_in(key_of[9], 71), 0),
        "queries": scatter_about(key_of[7], (QUERY_KEY_HEADS * KEY_CHANNELS,), 1.0, 6.0, ((0, 8),)),
        "out_gain": jnp.clip(1.0 + 0.18 * jax.random.normal(key_of[8], (QUERY_KEY_HEADS, VALUE_CHANNELS), jnp.float32), 0.1, 1.9),
    }


EPS = 1e-06
GATE_NORM = 16.0

def span_state(span_rows, span_drift, norm_gain, w_key, w_decay, w_value, decay_bias):
    rows_f32 = span_rows.astype(jnp.float32)
    inverse_rms = lax.rsqrt(lax.optimization_barrier(jnp.mean(rows_f32 * rows_f32, axis=1, keepdims=True)) + EPS)
    normed = (rows_f32 * inverse_rms * norm_gain[None, :]).astype(jnp.bfloat16)
    key_proj = jnp.dot(normed, w_key, preferred_element_type=jnp.float32).astype(jnp.bfloat16)
    gate_pre = jnp.dot(normed, w_decay, preferred_element_type=jnp.float32).astype(jnp.bfloat16)
    value_proj = jnp.dot(normed, w_value, preferred_element_type=jnp.float32).astype(jnp.bfloat16)
    log_decay = jax.nn.log_sigmoid(gate_pre.astype(jnp.float32) + decay_bias[None, :] + span_drift[:, None]) / GATE_NORM
    suffix = lax.cumsum(log_decay, axis=0, reverse=True)
    weighted = (key_proj.astype(jnp.float32) * jnp.exp(suffix - log_decay)).astype(jnp.bfloat16)
    partial_value = lax.dot_general(weighted, value_proj, (((0,), (0,)), ((), ())), preferred_element_type=jnp.float32)
    return (partial_value, suffix[0])

def reference(tokens, norm_gain, w_key, w_decay, w_value, decay_bias, gate_drift, queries, out_gain):
    span_rows = tokens.reshape(N_SP, SPAN, D)
    span_drift = gate_drift.reshape(N_SP, SPAN)

    def single_span(inputs):
        return span_state(inputs[0], inputs[1], norm_gain, w_key, w_decay, w_value, decay_bias)
    partials, span_total = lax.map(single_span, (span_rows, span_drift))
    later_sum = lax.cumsum(span_total, axis=0, reverse=True) - span_total
    matrix_state = lax.optimization_barrier(jnp.sum(jnp.exp(later_sum)[:, :, None] * partials, axis=0))
    state_cache = matrix_state.astype(jnp.bfloat16)
    query_of_head = queries.astype(jnp.float32).reshape(QUERY_KEY_HEADS, KEY_CHANNELS) * KEY_CHANNELS ** (-0.5)
    summed_read = jnp.einsum('gr,grs->gs', query_of_head, matrix_state.reshape(QUERY_KEY_HEADS, KEY_CHANNELS, VALUE_CHANNELS), precision=lax.Precision.HIGHEST)
    squares = lax.optimization_barrier(jnp.mean(summed_read * summed_read, axis=1, keepdims=True))
    first_read = summed_read * lax.rsqrt(squares + EPS) * out_gain
    return (state_cache, first_read)
```

```python
import functools

import jax
import jax.numpy as jnp
from jax import lax
from jax.experimental import pallas as pl
from jax.experimental.pallas import tpu as pltpu
from jax.sharding import PartitionSpec as P

QUERY_KEY_HEADS = 4
KEY_CHANNELS = 256
VALUE_CHANNELS = 512


EPS = 1e-06
GATE_NORM = 16.0


def body(tokens, norm_gain, w_key, w_decay, w_value, decay_bias, gate_drift, queries, out_gain):
    gathered = lax.all_gather(tokens, "tp", axis=1, tiled=True)
    rows_f32 = gathered.astype(jnp.float32)
    inverse_rms = lax.rsqrt(jnp.mean(rows_f32 * rows_f32, axis=1, keepdims=True) + EPS)
    normed = (rows_f32 * inverse_rms * norm_gain[None, :]).astype(jnp.bfloat16)
    key_proj = jnp.dot(normed, w_key, preferred_element_type=jnp.float32).astype(jnp.bfloat16)
    gate_pre = jnp.dot(normed, w_decay, preferred_element_type=jnp.float32).astype(jnp.bfloat16)
    value_proj = jnp.dot(normed, w_value, preferred_element_type=jnp.float32).astype(jnp.bfloat16)
    log_decay = (
        jax.nn.log_sigmoid(gate_pre.astype(jnp.float32) + decay_bias[None, :] + gate_drift[:, None])
        / GATE_NORM
    )
    suffix = lax.cumsum(log_decay, axis=0, reverse=True)
    weighted = (key_proj.astype(jnp.float32) * jnp.exp(suffix - log_decay)).astype(jnp.bfloat16)
    partial_value = lax.dot_general(
        weighted, value_proj, (((0,), (0,)), ((), ())), preferred_element_type=jnp.float32
    )
    total_decay = suffix[0]
    channels = partial_value.shape[0]
    span_count = lax.axis_size("sp")
    spread = jnp.broadcast_to(total_decay[None, :, None], (1, channels, span_count))
    blocks, totals = (
        lax.all_to_all(partial_value[None], "sp", split_axis=2, concat_axis=0, tiled=True),
        lax.all_to_all(spread, "sp", split_axis=2, concat_axis=0, tiled=True),
    )
    later_sum = lax.cumsum(totals, axis=0, reverse=True) - totals
    matrix_state = jnp.sum(jnp.exp(later_sum) * blocks, axis=0)
    state_cache = matrix_state.astype(jnp.bfloat16)
    channel_ids = lax.axis_index("tp") * channels + jnp.arange(channels, dtype=jnp.int32)
    owners = (channel_ids // KEY_CHANNELS)[:, None] == jnp.arange(QUERY_KEY_HEADS, dtype=jnp.int32)[
        None, :
    ]
    query_of_head = jnp.where(
        owners, queries.astype(jnp.float32)[:, None] * KEY_CHANNELS ** (-0.5), 0.0
    )
    part_read = lax.dot_general(
        query_of_head, matrix_state, (((0,), (0,)), ((), ())), precision=lax.Precision.HIGHEST
    )
    summed_read = lax.psum(part_read, "tp")
    squares = lax.psum(jnp.sum(summed_read * summed_read, axis=1), "sp")
    first_read = summed_read * lax.rsqrt(squares / VALUE_CHANNELS + EPS)[:, None] * out_gain
    return (state_cache, first_read)


PAIR = 2
LANES = 128
F32 = jnp.float32
BF16 = jnp.bfloat16


def dot(a, b):
    return jnp.dot(a, b, preferred_element_type=F32)


def kernel(n_sp, n_tp, query_scale, tokens, gain, wk, wd, wv, bias, drift, query, out_gain,
           state_out, read_out,
           tok, wbuf, wval, normed, val_t, biases, part_send, part_recv, tot_send, tot_recv, rd_send, rd_recv,
           load_sem, tok_s, tok_r, half_s, half_r, wz_s, w_r, wp_s, bias_s, bias_r,
           part_s, part_r, tot_s, tot_r, rd_s, rd_r):
    nz = n_tp // PAIR
    n = n_sp * n_tp
    s, t = lax.axis_index("sp"), lax.axis_index("tp")
    z, c = t // PAIR, t % PAIR
    me = s * n_tp + t
    rows = tok.shape[1]
    quarter = wbuf.shape[1] // n_sp
    vals = LANES

    def remote(src, dst, ssem, rsem, sp, tp):
        return pltpu.make_async_remote_copy(
            src_ref=src, dst_ref=dst, send_sem=ssem, recv_sem=rsem,
            device_id=(sp, tp), device_id_type=pl.DeviceIdType.MESH)

    loads = [
        pltpu.make_async_copy(wk, wbuf.at[z, :, 0:LANES], load_sem.at[0]),
        pltpu.make_async_copy(wd, wbuf.at[z, :, LANES:2 * LANES], load_sem.at[1]),
        pltpu.make_async_copy(wv, wval, load_sem.at[2]),
    ]
    for load in loads:
        load.start()

    barrier = pltpu.get_barrier_semaphore()

    def greet(d, carry):
        other = (me + d) % n
        pl.semaphore_signal(barrier, inc=1, device_id=(other // n_tp, other % n_tp),
                            device_id_type=pl.DeviceIdType.MESH)
        return carry
    lax.fori_loop(1, n, greet, 0)
    loads[0].wait()
    loads[1].wait()
    pl.semaphore_wait(barrier, n - 1)

    def w_slot(zo, q):
        return wbuf.at[zo, pl.ds(pl.multiple_of(q * quarter, LANES), quarter), :]

    def along(zo, dz, k):
        side = (dz + 1) // 2
        return remote(w_slot(zo, s), w_slot(zo, s), wz_s.at[side, k], w_r.at[zo, s],
                      s, (z + dz) * PAIR + c)

    def in_plane(zo, i):
        return remote(w_slot(zo, s), w_slot(zo, s), wp_s.at[zo, i - 1], w_r.at[zo, s],
                      (s + i) % n_sp, t)

    def to_column(i):
        zd = (z + i) % nz
        return remote(tokens.at[pl.ds(pl.multiple_of(zd * rows, LANES), rows), :], tok.at[t],
                      tok_s.at[i - 1], tok_r.at[t], s, zd * PAIR + c)

    def bias_to(i):
        return remote(bias, biases.at[z], bias_s.at[i - 1], bias_r.at[z], s, ((z + i) % nz) * PAIR + c)

    def to_pair(zo):
        return remote(tok.at[zo * PAIR + c], tok.at[zo * PAIR + c], half_s.at[zo],
                      half_r.at[zo], s, z * PAIR + 1 - c)

    for dz in (1, -1):
        @pl.when((z + dz >= 0) & (z + dz < nz))
        def _():
            along(z, dz, 0).start()
    tok_own = pltpu.make_async_copy(
        tokens.at[pl.ds(pl.multiple_of(z * rows, LANES), rows), :], tok.at[t], load_sem.at[0])
    tok_own.start()
    for i in range(1, nz):
        bias_to(i).start()
    far = nz // 2
    to_column(far).start()
    biases[z] = bias[...]
    tok_own.wait()
    to_pair(z).start()

    for k in range(1, nz):
        for dz in (1, -1):
            zo = z - k * dz

            @pl.when((zo >= 0) & (zo < nz))
            def _():
                along(zo, dz, 0).wait_recv()

                @pl.when((z + dz >= 0) & (z + dz < nz))
                def _():
                    along(zo, dz, k).start()
                for i in range(1, n_sp):
                    in_plane(zo, i).start()
        if k == 1:
            for i in range(1, nz):
                if i != far:
                    to_column(i).start()

    for i in [far] + [i for i in range(1, nz) if i != far]:
        zo = (z + nz - i) % nz
        pltpu.make_async_copy(tok.at[zo * PAIR + c], tok.at[zo * PAIR + c], tok_r.at[zo * PAIR + c]).wait()
        to_pair(zo).start()

    def got_pair(zo):
        other = zo * PAIR + 1 - c
        pltpu.make_async_copy(tok.at[other], tok.at[other], half_r.at[zo]).wait()
    for zo in range(nz):
        got_pair(zo)

    feats = tok.shape[2]
    squares = jnp.zeros((rows, LANES), F32)
    for b in range(n_tp):
        x = tok[b].astype(F32)
        for l in range(feats // LANES):
            y = x[:, l * LANES:(l + 1) * LANES]
            squares = squares + y * y
    inverse = lax.rsqrt(jnp.sum(squares, axis=1, keepdims=True) / (n_tp * feats) + EPS)
    for b in range(n_tp):
        cols = slice(b * feats, (b + 1) * feats)
        normed[:, cols] = (tok[b].astype(F32) * inverse * gain[:, cols]).astype(BF16)
    loads[2].wait()
    val_t[...] = dot(normed[...], wval[...]).T.astype(BF16)
    drift_col = jnp.broadcast_to(drift[z], (LANES, rows)).T
    tri = (lax.broadcasted_iota(jnp.int32, (rows, rows), 1)
           > lax.broadcasted_iota(jnp.int32, (rows, rows), 0)).astype(BF16)

    own = s * nz + z

    def part_to(zo, sd):
        return remote(part_send.at[zo, pl.ds(pl.multiple_of(sd * vals, vals), vals), :], part_recv.at[own],
                      part_s.at[zo, sd], part_r.at[own], sd, zo * PAIR + c)

    def tot_to(zo, sd):
        return remote(tot_send.at[zo], tot_recv.at[own], tot_s.at[zo, sd], tot_r.at[own],
                      sd, zo * PAIR + c)

    for i in range(1, nz):
        zo = (z + i) % nz
        pltpu.make_async_copy(biases.at[zo], biases.at[zo], bias_r.at[zo]).wait()

    def block(j, carry):
        zo = (z + j) % nz

        @pl.when(j > 0)
        def _():
            for i in range(1, n_sp):
                q = (s + i) % n_sp
                pltpu.make_async_copy(w_slot(zo, q), w_slot(zo, q), w_r.at[zo, q]).wait()
        proj = dot(normed[...], wbuf[zo])
        key = proj[:, :LANES].astype(BF16).astype(F32)
        gate = proj[:, LANES:].astype(BF16).astype(F32)
        u = gate + biases[zo] + drift_col
        log_decay = (jnp.minimum(u, 0.0) - jnp.log1p(jnp.exp(-jnp.abs(u)))) / GATE_NORM
        high = log_decay.astype(BF16)
        low = (log_decay - high.astype(F32)).astype(BF16)
        later = dot(tri, jnp.concatenate([high, low], axis=1))
        rest = later[:, :LANES] + later[:, LANES:]
        weighted = (key * jnp.exp(rest)).astype(BF16)
        tot_send[zo] = jnp.sum(log_decay, axis=0, keepdims=True)
        part_send[zo] = dot(val_t[...], weighted).astype(BF16)
        for i in range(1, n_sp):
            sd = (s + i) % n_sp
            part_to(zo, sd).start()
            tot_to(zo, sd).start()

        @pl.when(j > 0)
        def _():
            part_to(zo, s).start()
            tot_to(zo, s).start()
        return carry
    lax.fori_loop(0, nz, block, 0)
    part_recv[own] = part_send[z, pl.ds(pl.multiple_of(s * vals, vals), vals), :]
    tot_recv[own] = tot_send[z]

    def arrived(d, carry):
        src = (own + d) % (n_sp * nz)
        pltpu.make_async_copy(part_recv.at[src], part_recv.at[src], part_r.at[src]).wait()
        pltpu.make_async_copy(tot_recv.at[src], tot_recv.at[src], tot_r.at[src]).wait()
        return carry
    lax.fori_loop(1, n_sp * nz, arrived, 0)

    later = jnp.zeros((1, LANES), F32)
    total = jnp.zeros((vals, LANES), F32)
    for k in reversed(range(n_sp * nz)):
        total = total + jnp.exp(later) * part_recv[k].astype(F32)
        later = later + tot_recv[k]
    state_out[...] = total.T.astype(BF16)
    scaled = query[...].astype(F32) * query_scale
    rd_send[...] = jnp.sum((total * scaled).T, axis=0, keepdims=True)
    rd_recv[me] = rd_send[...]

    def read_to(d):
        other = (me + d) % n
        return remote(rd_send, rd_recv.at[me], rd_s.at[d], rd_r.at[me], other // n_tp, other % n_tp)

    def send_read(d, carry):
        read_to(d).start()
        return carry
    lax.fori_loop(1, n, send_read, 0)

    for dz in (1, -1):
        for k in range(nz - 1):
            zo = z - k * dz

            @pl.when((zo >= 0) & (zo < nz) & (z + dz >= 0) & (z + dz < nz))
            def _():
                along(zo, dz, k).wait_send()
    for i in range(1, nz):
        to_column(i).wait_send()
        bias_to(i).wait_send()
        for q in range(1, n_sp):
            in_plane((z + i) % nz, q).wait_send()
    for zo in range(nz):
        to_pair(zo).wait_send()

    def sent(j, carry):
        zo = (z + j) % nz
        for i in range(1, n_sp):
            sd = (s + i) % n_sp
            part_to(zo, sd).wait_send()
            tot_to(zo, sd).wait_send()

        @pl.when(j > 0)
        def _():
            part_to(zo, s).wait_send()
            tot_to(zo, s).wait_send()
        return carry
    lax.fori_loop(0, nz, sent, 0)

    def read_from(d, carry):
        src = (me + d) % n
        pltpu.make_async_copy(rd_recv.at[src], rd_recv.at[src], rd_r.at[src]).wait()
        return carry
    lax.fori_loop(1, n, read_from, 0)

    def read_sent(d, carry):
        read_to(d).wait_send()
        return carry
    lax.fori_loop(1, n, read_sent, 0)

    heads = read_out.shape[0]
    per_head = n_tp // heads

    def head_row(sp, h):
        row = rd_recv[sp * n_tp + h * per_head]
        for i in range(1, per_head):
            row = row + rd_recv[sp * n_tp + h * per_head + i]
        return row
    for h in range(heads):
        squared = jnp.zeros((1, LANES), F32)
        for sp in range(n_sp):
            row = head_row(sp, h)
            squared = squared + row * row
        mean = jnp.sum(squared, axis=1, keepdims=True) / (n_sp * vals)
        read_out[h:h + 1, :] = head_row(s, h) * lax.rsqrt(mean + EPS) * out_gain[h:h + 1, :]


def fused_body(tokens, norm_gain, w_key, w_decay, w_value, decay_bias, gate_drift, queries, out_gain):
    n_sp, n_tp = lax.axis_size("sp"), lax.axis_size("tp")
    nz = n_tp // PAIR
    span, feats = tokens.shape
    width = feats * n_tp
    rows = span // nz
    channels = w_key.shape[1]
    vals = out_gain.shape[1]
    values = w_value.shape[1]
    vmem = pl.BlockSpec(memory_space=pltpu.VMEM)
    hbm = pl.BlockSpec(memory_space=pl.ANY)
    dma = pltpu.SemaphoreType.DMA
    return pl.pallas_call(
        functools.partial(kernel, n_sp, n_tp, KEY_CHANNELS ** (-0.5)),
        out_shape=(jax.ShapeDtypeStruct((channels, vals), BF16),
                   jax.ShapeDtypeStruct(out_gain.shape, F32)),
        in_specs=[vmem, vmem, hbm, hbm, hbm, vmem, vmem, vmem, vmem],
        out_specs=(vmem, vmem),
        scratch_shapes=[
            pltpu.VMEM((n_tp, rows, feats), BF16),
            pltpu.VMEM((nz, width, 2 * channels), BF16),
            pltpu.VMEM((width, values), BF16),
            pltpu.VMEM((rows, width), BF16),
            pltpu.VMEM((values, rows), BF16),
            pltpu.VMEM((nz, 1, channels), F32),
            pltpu.VMEM((nz, values, channels), BF16),
            pltpu.VMEM((n_sp * nz, vals, channels), BF16),
            pltpu.VMEM((nz, 1, channels), F32),
            pltpu.VMEM((n_sp * nz, 1, channels), F32),
            pltpu.VMEM((1, vals), F32),
            pltpu.VMEM((n_sp * n_tp, 1, vals), F32),
            dma((3,)),
            dma((nz - 1,)), dma((n_tp,)),
            dma((nz,)), dma((nz,)),
            dma((2, nz)), dma((nz, n_sp)), dma((nz, n_sp - 1)),
            dma((nz - 1,)), dma((nz,)),
            dma((nz, n_sp)), dma((n_sp * nz,)),
            dma((nz, n_sp)), dma((n_sp * nz,)),
            dma((n_sp * n_tp,)), dma((n_sp * n_tp,)),
        ],
        compiler_params=pltpu.CompilerParams(
            collective_id=0, has_side_effects=True, vmem_limit_bytes=48 * 1024 * 1024),
    )(tokens, norm_gain.reshape(1, width), w_key, w_decay, w_value, decay_bias.reshape(1, channels),
      gate_drift.reshape(nz, 1, rows), queries.reshape(1, channels), out_gain)


def fits(tokens, w_key, w_value, out_gain, n_tp):
    nz = n_tp // PAIR
    return (n_tp % PAIR == 0 and nz > 1 and tokens.shape[0] % (nz * LANES) == 0
            and tokens.shape[1] % LANES == 0 and w_key.shape[1] == LANES and out_gain.shape[1] == LANES
            and n_tp % out_gain.shape[0] == 0)


def choose(tokens, norm_gain, w_key, w_decay, w_value, decay_bias, gate_drift, queries, out_gain):
    args = (tokens, norm_gain, w_key, w_decay, w_value, decay_bias, gate_drift, queries, out_gain)
    if fits(tokens, w_key, w_value, out_gain, lax.axis_size("tp")):
        return fused_body(*args)
    return body(*args)


def solution(mesh):
    return jax.shard_map(
        choose,
        mesh=mesh,
        in_specs=(
            P("sp", "tp"),
            P(),
            P(None, "tp"),
            P(None, "tp"),
            P(),
            P("tp"),
            P("sp"),
            P("tp"),
            P(None, "sp"),
        ),
        out_specs=(P("tp", "sp"), P(None, "sp")),
        check_vma=False,
    )
```

```python
import functools

import jax
import jax.numpy as jnp
from jax import lax
from jax.experimental import pallas as pl
from jax.experimental.pallas import tpu as pltpu
from jax.sharding import PartitionSpec as P

QUERY_KEY_HEADS = 4
KEY_CHANNELS = 256
VALUE_CHANNELS = 512


EPS = 1e-06
GATE_NORM = 16.0


def body(tokens, norm_gain, w_key, w_decay, w_value, decay_bias, gate_drift, queries, out_gain):
    gathered = lax.all_gather(tokens, "tp", axis=1, tiled=True)
    rows_f32 = gathered.astype(jnp.float32)
    inverse_rms = lax.rsqrt(jnp.mean(rows_f32 * rows_f32, axis=1, keepdims=True) + EPS)
    normed = (rows_f32 * inverse_rms * norm_gain[None, :]).astype(jnp.bfloat16)
    key_proj = jnp.dot(normed, w_key, preferred_element_type=jnp.float32).astype(jnp.bfloat16)
    gate_pre = jnp.dot(normed, w_decay, preferred_element_type=jnp.float32).astype(jnp.bfloat16)
    value_proj = jnp.dot(normed, w_value, preferred_element_type=jnp.float32).astype(jnp.bfloat16)
    log_decay = (
        jax.nn.log_sigmoid(gate_pre.astype(jnp.float32) + decay_bias[None, :] + gate_drift[:, None])
        / GATE_NORM
    )
    suffix = lax.cumsum(log_decay, axis=0, reverse=True)
    weighted = (key_proj.astype(jnp.float32) * jnp.exp(suffix - log_decay)).astype(jnp.bfloat16)
    partial_value = lax.dot_general(
        weighted, value_proj, (((0,), (0,)), ((), ())), preferred_element_type=jnp.float32
    )
    total_decay = suffix[0]
    channels = partial_value.shape[0]
    span_count = lax.axis_size("sp")
    spread = jnp.broadcast_to(total_decay[None, :, None], (1, channels, span_count))
    blocks, totals = (
        lax.all_to_all(partial_value[None], "sp", split_axis=2, concat_axis=0, tiled=True),
        lax.all_to_all(spread, "sp", split_axis=2, concat_axis=0, tiled=True),
    )
    later_sum = lax.cumsum(totals, axis=0, reverse=True) - totals
    matrix_state = jnp.sum(jnp.exp(later_sum) * blocks, axis=0)
    state_cache = matrix_state.astype(jnp.bfloat16)
    channel_ids = lax.axis_index("tp") * channels + jnp.arange(channels, dtype=jnp.int32)
    owners = (channel_ids // KEY_CHANNELS)[:, None] == jnp.arange(QUERY_KEY_HEADS, dtype=jnp.int32)[
        None, :
    ]
    query_of_head = jnp.where(
        owners, queries.astype(jnp.float32)[:, None] * KEY_CHANNELS ** (-0.5), 0.0
    )
    part_read = lax.dot_general(
        query_of_head, matrix_state, (((0,), (0,)), ((), ())), precision=lax.Precision.HIGHEST
    )
    summed_read = lax.psum(part_read, "tp")
    squares = lax.psum(jnp.sum(summed_read * summed_read, axis=1), "sp")
    first_read = summed_read * lax.rsqrt(squares / VALUE_CHANNELS + EPS)[:, None] * out_gain
    return (state_cache, first_read)


PAIR = 2
LANES = 128
PLANE = 4
VMEM_BYTES = 67_000_000
F32 = jnp.float32
BF16 = jnp.bfloat16


def dot(a, b):
    return jnp.dot(a, b, preferred_element_type=F32)


def kernel(n_sp, n_tp, query_scale, tokens_in, gain_in, wk, wd, wv, bias_in, drift_in, query_in, out_gain_in,
           state_out, read_out,
           tokens, gain, drift, query, out_gain, tok, wbuf, wval, normed, val_t, biases, part_send, part_recv, tot_send, tot_recv, rd_send, rd_recv,
           load_sem, tok_s, tok_r, half_s, half_r, wz_s, w_r, wp_s, bias_s, bias_r,
           part_s, part_r, tot_s, tot_r, rd_s, rd_r):
    nz = n_tp // PAIR
    n = n_sp * n_tp
    s, t = lax.axis_index("sp"), lax.axis_index("tp")
    z, c = t // PAIR, t % PAIR
    me = s * n_tp + t
    rows = tok.shape[1]
    quarter = wbuf.shape[1] // n_sp
    vals = LANES

    def remote(src, dst, ssem, rsem, sp, tp):
        return pltpu.make_async_remote_copy(
            src_ref=src, dst_ref=dst, send_sem=ssem, recv_sem=rsem,
            device_id=(sp, tp), device_id_type=pl.DeviceIdType.MESH)

    loads = [
        pltpu.make_async_copy(wk, wbuf.at[z, :, 0:LANES], load_sem.at[0]),
        pltpu.make_async_copy(wd, wbuf.at[z, :, LANES:2 * LANES], load_sem.at[1]),
        pltpu.make_async_copy(tokens_in, tokens, load_sem.at[2]),
        pltpu.make_async_copy(bias_in, biases.at[z], load_sem.at[3]),
        pltpu.make_async_copy(gain_in, gain, load_sem.at[4]),
        pltpu.make_async_copy(drift_in, drift, load_sem.at[5]),
        pltpu.make_async_copy(query_in, query, load_sem.at[6]),
        pltpu.make_async_copy(out_gain_in, out_gain, load_sem.at[7]),
        pltpu.make_async_copy(wv, wval, load_sem.at[8]),
    ]
    for load in loads:
        load.start()

    barrier = pltpu.get_barrier_semaphore()

    def greet(d, carry):
        other = (me + d) % n
        pl.semaphore_signal(barrier, inc=1, device_id=(other // n_tp, other % n_tp),
                            device_id_type=pl.DeviceIdType.MESH)
        return carry
    lax.fori_loop(1, n, greet, 0)
    for load in loads[:4]:
        load.wait()
    pl.semaphore_wait(barrier, n - 1)

    def w_slot(zo, q):
        return wbuf.at[zo, pl.ds(pl.multiple_of(q * quarter, LANES), quarter), :]

    def along(zo, dz, k):
        side = (dz + 1) // 2
        return remote(w_slot(zo, s), w_slot(zo, s), wz_s.at[side, k], w_r.at[zo, s],
                      s, (z + dz) * PAIR + c)

    x_bit, y_bit = s % 2, s // 2
    x_peer, y_peer = y_bit * 2 + 1 - x_bit, (1 - y_bit) * 2 + x_bit
    corner = (1 - y_bit) * 2 + 1 - x_bit
    peers = (x_peer, y_peer)

    def in_plane(zo, i):
        return remote(w_slot(zo, s), w_slot(zo, s), wp_s.at[zo, i], w_r.at[zo, s], peers[i], t)

    def relay(zo, i):
        half = quarter // 2
        q = peers[1 - i]
        part = wbuf.at[zo, pl.ds(pl.multiple_of(q * quarter + i * half, LANES), half), :]
        return remote(part, part, wp_s.at[zo, 2 + i], w_r.at[zo, q], peers[i], t)

    def relay_both(zo):
        for i in range(2):
            q = peers[1 - i]
            pltpu.make_async_copy(w_slot(zo, q), w_slot(zo, q), w_r.at[zo, q]).wait()
            relay(zo, i).start()

    def to_column(i):
        zd = (z + i) % nz
        return remote(tokens.at[pl.ds(pl.multiple_of(zd * rows, LANES), rows), :], tok.at[t],
                      tok_s.at[i - 1], tok_r.at[t], s, zd * PAIR + c)

    def bias_to(i):
        return remote(biases.at[z], biases.at[z], bias_s.at[i - 1], bias_r.at[z], s, ((z + i) % nz) * PAIR + c)

    def to_pair(zo):
        return remote(tok.at[zo * PAIR + c], tok.at[zo * PAIR + c], half_s.at[zo],
                      half_r.at[zo], s, z * PAIR + 1 - c)

    for dz in (1, -1):
        @pl.when((z + dz >= 0) & (z + dz < nz))
        def _():
            along(z, dz, 0).start()
    tok_own = pltpu.make_async_copy(
        tokens.at[pl.ds(pl.multiple_of(z * rows, LANES), rows), :], tok.at[t], load_sem.at[0])
    tok_own.start()
    for i in range(1, nz):
        bias_to(i).start()
    far = nz // 2
    to_column(far).start()
    tok_own.wait()
    to_pair(z).start()

    def relay_step(k):
        for dz in (1, -1):
            zo = z - k * dz

            @pl.when((zo >= 0) & (zo < nz))
            def _():
                relay_both(zo)

    for k in range(1, nz):
        for dz in (1, -1):
            zo = z - k * dz

            @pl.when((zo >= 0) & (zo < nz))
            def _():
                along(zo, dz, 0).wait_recv()

                @pl.when((z + dz >= 0) & (z + dz < nz))
                def _():
                    along(zo, dz, k).start()
                for i in range(2):
                    in_plane(zo, i).start()
        if k > 1:
            relay_step(k - 1)
        if k == 1:
            for i in range(1, nz):
                if i != far:
                    to_column(i).start()

    for i in [far] + [i for i in range(1, nz) if i != far]:
        zo = (z + nz - i) % nz
        pltpu.make_async_copy(tok.at[zo * PAIR + c], tok.at[zo * PAIR + c], tok_r.at[zo * PAIR + c]).wait()
        to_pair(zo).start()

    def got_pair(zo):
        other = zo * PAIR + 1 - c
        pltpu.make_async_copy(tok.at[other], tok.at[other], half_r.at[zo]).wait()
    for zo in range(nz):
        got_pair(zo)

    for load in loads[4:8]:
        load.wait()
    feats = tok.shape[2]
    squares = jnp.zeros((rows, LANES), F32)
    for b in range(n_tp):
        x = tok[b].astype(F32)
        for l in range(feats // LANES):
            y = x[:, l * LANES:(l + 1) * LANES]
            squares = squares + y * y
    inverse = lax.rsqrt(jnp.sum(squares, axis=1, keepdims=True) / (n_tp * feats) + EPS)
    for b in range(n_tp):
        cols = slice(b * feats, (b + 1) * feats)
        normed[:, cols] = (tok[b].astype(F32) * inverse * gain[:, cols]).astype(BF16)
    relay_step(nz - 1)
    loads[8].wait()
    val_t[...] = dot(normed[...], wval[...]).T.astype(BF16)
    drift_col = jnp.broadcast_to(drift[z], (LANES, rows)).T
    tri = (lax.broadcasted_iota(jnp.int32, (rows, rows), 1)
           > lax.broadcasted_iota(jnp.int32, (rows, rows), 0)).astype(BF16)

    own = s * nz + z

    def part_to(zo, sd):
        return remote(part_send.at[zo, pl.ds(pl.multiple_of(sd * vals, vals), vals), :], part_recv.at[own],
                      part_s.at[zo, sd], part_r.at[own], sd, zo * PAIR + c)

    def tot_to(zo, sd):
        return remote(tot_send.at[zo], tot_recv.at[own], tot_s.at[zo, sd], tot_r.at[own],
                      sd, zo * PAIR + c)

    for i in range(1, nz):
        zo = (z + i) % nz
        pltpu.make_async_copy(biases.at[zo], biases.at[zo], bias_r.at[zo]).wait()

    def nearest(j):
        low = z < nz // 2
        edge = jnp.where(low, z, nz - 1 - z)
        at = jnp.where(j == 0, edge, jnp.where(j - 1 < edge, j - 1, j))
        return jnp.where(low, at, nz - 1 - at)

    def block(j, carry):
        zo = nearest(j)

        @pl.when(j > 0)
        def _():
            pltpu.make_async_copy(w_slot(zo, corner), w_slot(zo, corner), w_r.at[zo, corner]).wait()
        proj = dot(normed[...], wbuf[zo])
        key = proj[:, :LANES].astype(BF16).astype(F32)
        gate = proj[:, LANES:].astype(BF16).astype(F32)
        u = gate + biases[zo] + drift_col
        log_decay = (jnp.minimum(u, 0.0) - jnp.log1p(jnp.exp(-jnp.abs(u)))) / GATE_NORM
        high = log_decay.astype(BF16)
        low = (log_decay - high.astype(F32)).astype(BF16)
        later = dot(tri, jnp.concatenate([high, low], axis=1))
        rest = later[:, :LANES] + later[:, LANES:]
        weighted = (key * jnp.exp(rest)).astype(BF16)
        tot_send[zo] = jnp.sum(log_decay, axis=0, keepdims=True)
        part_send[zo] = dot(val_t[...], weighted).astype(BF16)
        for i in range(1, n_sp):
            sd = (s + i) % n_sp
            part_to(zo, sd).start()
            tot_to(zo, sd).start()

        @pl.when(j > 0)
        def _():
            part_to(zo, s).start()
            tot_to(zo, s).start()
        return carry
    lax.fori_loop(0, nz, block, 0)
    part_recv[own] = part_send[z, pl.ds(pl.multiple_of(s * vals, vals), vals), :]
    tot_recv[own] = tot_send[z]

    def arrived(d, carry):
        src = (own + d) % (n_sp * nz)
        pltpu.make_async_copy(part_recv.at[src], part_recv.at[src], part_r.at[src]).wait()
        pltpu.make_async_copy(tot_recv.at[src], tot_recv.at[src], tot_r.at[src]).wait()
        return carry
    lax.fori_loop(1, n_sp * nz, arrived, 0)

    later = jnp.zeros((1, LANES), F32)
    total = jnp.zeros((vals, LANES), F32)
    for k in reversed(range(n_sp * nz)):
        total = total + jnp.exp(later) * part_recv[k].astype(F32)
        later = later + tot_recv[k]
    scaled = query[...].astype(F32) * query_scale
    rd_send[...] = jnp.sum((total * scaled).T, axis=0, keepdims=True)
    rd_recv[me] = rd_send[...]

    def read_to(d):
        other = (me + d) % n
        return remote(rd_send, rd_recv.at[me], rd_s.at[d], rd_r.at[me], other // n_tp, other % n_tp)

    def send_read(d, carry):
        read_to(d).start()
        return carry
    lax.fori_loop(1, n, send_read, 0)
    state_out[...] = total.T.astype(BF16)

    for dz in (1, -1):
        for k in range(nz - 1):
            zo = z - k * dz

            @pl.when((zo >= 0) & (zo < nz) & (z + dz >= 0) & (z + dz < nz))
            def _():
                along(zo, dz, k).wait_send()
    for i in range(1, nz):
        to_column(i).wait_send()
        bias_to(i).wait_send()
        for j in range(2):
            in_plane((z + i) % nz, j).wait_send()
            relay((z + i) % nz, j).wait_send()
    for zo in range(nz):
        to_pair(zo).wait_send()

    def sent(j, carry):
        zo = nearest(j)
        for i in range(1, n_sp):
            sd = (s + i) % n_sp
            part_to(zo, sd).wait_send()
            tot_to(zo, sd).wait_send()

        @pl.when(j > 0)
        def _():
            part_to(zo, s).wait_send()
            tot_to(zo, s).wait_send()
        return carry
    lax.fori_loop(0, nz, sent, 0)

    def read_from(d, carry):
        src = (me + d) % n
        pltpu.make_async_copy(rd_recv.at[src], rd_recv.at[src], rd_r.at[src]).wait()
        return carry
    lax.fori_loop(1, n, read_from, 0)

    def read_sent(d, carry):
        read_to(d).wait_send()
        return carry
    lax.fori_loop(1, n, read_sent, 0)

    heads = read_out.shape[0]
    per_head = n_tp // heads

    def head_row(sp, h):
        row = rd_recv[sp * n_tp + h * per_head]
        for i in range(1, per_head):
            row = row + rd_recv[sp * n_tp + h * per_head + i]
        return row
    for h in range(heads):
        squared = jnp.zeros((1, LANES), F32)
        for sp in range(n_sp):
            row = head_row(sp, h)
            squared = squared + row * row
        mean = jnp.sum(squared, axis=1, keepdims=True) / (n_sp * vals)
        read_out[h:h + 1, :] = head_row(s, h) * lax.rsqrt(mean + EPS) * out_gain[h:h + 1, :]


def fused_body(tokens, norm_gain, w_key, w_decay, w_value, decay_bias, gate_drift, queries, out_gain):
    n_sp, n_tp = lax.axis_size("sp"), lax.axis_size("tp")
    nz = n_tp // PAIR
    span, feats = tokens.shape
    width = feats * n_tp
    rows = span // nz
    channels = w_key.shape[1]
    vals = out_gain.shape[1]
    values = w_value.shape[1]
    vmem = pl.BlockSpec(memory_space=pltpu.VMEM)
    hbm = pl.BlockSpec(memory_space=pltpu.HBM)
    dma = pltpu.SemaphoreType.DMA
    return pl.pallas_call(
        functools.partial(kernel, n_sp, n_tp, KEY_CHANNELS ** (-0.5)),
        out_shape=(jax.ShapeDtypeStruct((channels, vals), BF16),
                   jax.ShapeDtypeStruct(out_gain.shape, F32)),
        in_specs=[hbm] * 9,
        out_specs=(vmem, vmem),
        scratch_shapes=[
            pltpu.VMEM(tokens.shape, BF16),
            pltpu.VMEM((1, width), F32),
            pltpu.VMEM((nz, 1, rows), F32),
            pltpu.VMEM((1, channels), BF16),
            pltpu.VMEM(out_gain.shape, F32),
            pltpu.VMEM((n_tp, rows, feats), BF16),
            pltpu.VMEM((nz, width, 2 * channels), BF16),
            pltpu.VMEM((width, values), BF16),
            pltpu.VMEM((rows, width), BF16),
            pltpu.VMEM((values, rows), BF16),
            pltpu.VMEM((nz, 1, channels), F32),
            pltpu.VMEM((nz, values, channels), BF16),
            pltpu.VMEM((n_sp * nz, vals, channels), BF16),
            pltpu.VMEM((nz, 1, channels), F32),
            pltpu.VMEM((n_sp * nz, 1, channels), F32),
            pltpu.VMEM((1, vals), F32),
            pltpu.VMEM((n_sp * n_tp, 1, vals), F32),
            dma((9,)),
            dma((nz - 1,)), dma((n_tp,)),
            dma((nz,)), dma((nz,)),
            dma((2, nz)), dma((nz, n_sp)), dma((nz, 4)),
            dma((nz - 1,)), dma((nz,)),
            dma((nz, n_sp)), dma((n_sp * nz,)),
            dma((nz, n_sp)), dma((n_sp * nz,)),
            dma((n_sp * n_tp,)), dma((n_sp * n_tp,)),
        ],
        compiler_params=pltpu.CompilerParams(
            collective_id=0, has_side_effects=True, vmem_limit_bytes=VMEM_BYTES),
    )(tokens, norm_gain.reshape(1, width), w_key, w_decay, w_value, decay_bias.reshape(1, channels),
      gate_drift.reshape(nz, 1, rows), queries.reshape(1, channels), out_gain)


def fits(tokens, w_key, w_value, out_gain, n_tp):
    nz = n_tp // PAIR
    return (lax.axis_size("sp") == PLANE and n_tp % PAIR == 0 and nz > 1 and tokens.shape[0] % (nz * LANES) == 0
            and tokens.shape[1] % LANES == 0 and w_key.shape[1] == LANES and out_gain.shape[1] == LANES
            and n_tp % out_gain.shape[0] == 0)


def choose(tokens, norm_gain, w_key, w_decay, w_value, decay_bias, gate_drift, queries, out_gain):
    args = (tokens, norm_gain, w_key, w_decay, w_value, decay_bias, gate_drift, queries, out_gain)
    if fits(tokens, w_key, w_value, out_gain, lax.axis_size("tp")):
        return fused_body(*args)
    return body(*args)


def solution(mesh):
    return jax.shard_map(
        choose,
        mesh=mesh,
        in_specs=(
            P("sp", "tp"),
            P(),
            P(None, "tp"),
            P(None, "tp"),
            P(),
            P("tp"),
            P("sp"),
            P("tp"),
            P(None, "sp"),
        ),
        out_specs=(P("tp", "sp"), P(None, "sp")),
        check_vma=False,
    )
```

```python
import functools

import jax
import jax.numpy as jnp
from jax import lax
from jax.experimental import pallas as pl
from jax.experimental.pallas import tpu as pltpu
from jax.sharding import PartitionSpec as P

QUERY_KEY_HEADS = 4
KEY_CHANNELS = 256
VALUE_CHANNELS = 512


EPS = 1e-06
GATE_NORM = 16.0


def body(tokens, norm_gain, w_key, w_decay, w_value, decay_bias, gate_drift, queries, out_gain):
    gathered = lax.all_gather(tokens, "tp", axis=1, tiled=True)
    rows_f32 = gathered.astype(jnp.float32)
    inverse_rms = lax.rsqrt(jnp.mean(rows_f32 * rows_f32, axis=1, keepdims=True) + EPS)
    normed = (rows_f32 * inverse_rms * norm_gain[None, :]).astype(jnp.bfloat16)
    key_proj = jnp.dot(normed, w_key, preferred_element_type=jnp.float32).astype(jnp.bfloat16)
    gate_pre = jnp.dot(normed, w_decay, preferred_element_type=jnp.float32).astype(jnp.bfloat16)
    value_proj = jnp.dot(normed, w_value, preferred_element_type=jnp.float32).astype(jnp.bfloat16)
    log_decay = (
        jax.nn.log_sigmoid(gate_pre.astype(jnp.float32) + decay_bias[None, :] + gate_drift[:, None])
        / GATE_NORM
    )
    suffix = lax.cumsum(log_decay, axis=0, reverse=True)
    weighted = (key_proj.astype(jnp.float32) * jnp.exp(suffix - log_decay)).astype(jnp.bfloat16)
    partial_value = lax.dot_general(
        weighted, value_proj, (((0,), (0,)), ((), ())), preferred_element_type=jnp.float32
    )
    total_decay = suffix[0]
    channels = partial_value.shape[0]
    span_count = lax.axis_size("sp")
    spread = jnp.broadcast_to(total_decay[None, :, None], (1, channels, span_count))
    blocks, totals = (
        lax.all_to_all(partial_value[None], "sp", split_axis=2, concat_axis=0, tiled=True),
        lax.all_to_all(spread, "sp", split_axis=2, concat_axis=0, tiled=True),
    )
    later_sum = lax.cumsum(totals, axis=0, reverse=True) - totals
    matrix_state = jnp.sum(jnp.exp(later_sum) * blocks, axis=0)
    state_cache = matrix_state.astype(jnp.bfloat16)
    channel_ids = lax.axis_index("tp") * channels + jnp.arange(channels, dtype=jnp.int32)
    owners = (channel_ids // KEY_CHANNELS)[:, None] == jnp.arange(QUERY_KEY_HEADS, dtype=jnp.int32)[
        None, :
    ]
    query_of_head = jnp.where(
        owners, queries.astype(jnp.float32)[:, None] * KEY_CHANNELS ** (-0.5), 0.0
    )
    part_read = lax.dot_general(
        query_of_head, matrix_state, (((0,), (0,)), ((), ())), precision=lax.Precision.HIGHEST
    )
    summed_read = lax.psum(part_read, "tp")
    squares = lax.psum(jnp.sum(summed_read * summed_read, axis=1), "sp")
    first_read = summed_read * lax.rsqrt(squares / VALUE_CHANNELS + EPS)[:, None] * out_gain
    return (state_cache, first_read)


PAIR = 2
LANES = 128
PLANE = 4
VMEM_BYTES = 67_000_000
F32 = jnp.float32
BF16 = jnp.bfloat16


def dot(a, b):
    return jnp.dot(a, b, preferred_element_type=F32)


def kernel(n_sp, n_tp, query_scale, tokens_in, gain_in, wk, wd, wv, bias_in, drift_in, query_in, out_gain_in,
           state_out, read_out,
           tokens, gain, drift, query, out_gain, tok, wbuf, wval, normed, val_t, biases, part_send, part_recv, tot_send, tot_recv, rd_send, rd_recv,
           load_sem, tok_s, tok_r, half_s, half_r, wz_s, w_r, wp_s, bias_s, bias_r,
           part_s, part_r, tot_s, tot_r, rd_s, rd_r):
    nz = n_tp // PAIR
    n = n_sp * n_tp
    s, t = lax.axis_index("sp"), lax.axis_index("tp")
    z, c = t // PAIR, t % PAIR
    me = s * n_tp + t
    rows = tok.shape[1]
    quarter = wbuf.shape[1] // n_sp
    vals = LANES

    def remote(src, dst, ssem, rsem, sp, tp):
        return pltpu.make_async_remote_copy(
            src_ref=src, dst_ref=dst, send_sem=ssem, recv_sem=rsem,
            device_id=(sp, tp), device_id_type=pl.DeviceIdType.MESH)

    loads = [
        pltpu.make_async_copy(wk, wbuf.at[z, :, 0:LANES], load_sem.at[0]),
        pltpu.make_async_copy(wd, wbuf.at[z, :, LANES:2 * LANES], load_sem.at[1]),
        pltpu.make_async_copy(tokens_in, tokens, load_sem.at[2]),
        pltpu.make_async_copy(bias_in, biases.at[z], load_sem.at[3]),
        pltpu.make_async_copy(gain_in, gain, load_sem.at[4]),
        pltpu.make_async_copy(drift_in, drift, load_sem.at[5]),
        pltpu.make_async_copy(query_in, query, load_sem.at[6]),
        pltpu.make_async_copy(out_gain_in, out_gain, load_sem.at[7]),
        pltpu.make_async_copy(wv, wval, load_sem.at[8]),
    ]
    for load in loads:
        load.start()

    barrier = pltpu.get_barrier_semaphore()

    def greet(d, carry):
        other = (me + d) % n
        pl.semaphore_signal(barrier, inc=1, device_id=(other // n_tp, other % n_tp),
                            device_id_type=pl.DeviceIdType.MESH)
        return carry
    lax.fori_loop(1, n, greet, 0)
    for load in loads[:4]:
        load.wait()
    pl.semaphore_wait(barrier, n - 1)

    def w_slot(zo, q):
        return wbuf.at[zo, pl.ds(pl.multiple_of(q * quarter, LANES), quarter), :]

    def along(zo, dz, k):
        side = (dz + 1) // 2
        return remote(w_slot(zo, s), w_slot(zo, s), wz_s.at[side, k], w_r.at[zo, s],
                      s, (z + dz) * PAIR + c)

    x_bit, y_bit = s % 2, s // 2
    x_peer, y_peer = y_bit * 2 + 1 - x_bit, (1 - y_bit) * 2 + x_bit
    corner = (1 - y_bit) * 2 + 1 - x_bit
    peers = (x_peer, y_peer)

    def in_plane(zo, i):
        return remote(w_slot(zo, s), w_slot(zo, s), wp_s.at[zo, i], w_r.at[zo, s], peers[i], t)

    def relay(zo, i):
        half = quarter // 2
        q = peers[1 - i]
        part = wbuf.at[zo, pl.ds(pl.multiple_of(q * quarter + i * half, LANES), half), :]
        return remote(part, part, wp_s.at[zo, 2 + i], w_r.at[zo, q], peers[i], t)

    def relay_both(zo):
        for i in range(2):
            q = peers[1 - i]
            pltpu.make_async_copy(w_slot(zo, q), w_slot(zo, q), w_r.at[zo, q]).wait()
            relay(zo, i).start()

    def to_column(i):
        zd = (z + i) % nz
        return remote(tokens.at[pl.ds(pl.multiple_of(zd * rows, LANES), rows), :], tok.at[t],
                      tok_s.at[i - 1], tok_r.at[t], s, zd * PAIR + c)

    def bias_to(i):
        return remote(biases.at[z], biases.at[z], bias_s.at[i - 1], bias_r.at[z], s, ((z + i) % nz) * PAIR + c)

    def to_pair(zo):
        return remote(tok.at[zo * PAIR + c], tok.at[zo * PAIR + c], half_s.at[zo],
                      half_r.at[zo], s, z * PAIR + 1 - c)

    for dz in (1, -1):
        @pl.when((z + dz >= 0) & (z + dz < nz))
        def _():
            along(z, dz, 0).start()
    tok_own = pltpu.make_async_copy(
        tokens.at[pl.ds(pl.multiple_of(z * rows, LANES), rows), :], tok.at[t], load_sem.at[0])
    tok_own.start()
    for i in range(1, nz):
        bias_to(i).start()
    far = nz // 2
    to_column(far).start()
    tok_own.wait()
    to_pair(z).start()

    def relay_step(k):
        for dz in (1, -1):
            zo = z - k * dz

            @pl.when((zo >= 0) & (zo < nz))
            def _():
                relay_both(zo)

    for k in range(1, nz):
        if k > 1:
            relay_step(k - 1)
        for dz in (1, -1):
            zo = z - k * dz

            @pl.when((zo >= 0) & (zo < nz))
            def _():
                along(zo, dz, 0).wait_recv()

                @pl.when((z + dz >= 0) & (z + dz < nz))
                def _():
                    along(zo, dz, k).start()
                for i in range(2):
                    in_plane(zo, i).start()
        if k == 1:
            for i in range(1, nz):
                if i != far:
                    to_column(i).start()

    for i in [far] + [i for i in range(1, nz) if i != far]:
        zo = (z + nz - i) % nz
        pltpu.make_async_copy(tok.at[zo * PAIR + c], tok.at[zo * PAIR + c], tok_r.at[zo * PAIR + c]).wait()
        to_pair(zo).start()

    def got_pair(zo):
        other = zo * PAIR + 1 - c
        pltpu.make_async_copy(tok.at[other], tok.at[other], half_r.at[zo]).wait()
    for zo in range(nz):
        got_pair(zo)

    for load in loads[4:8]:
        load.wait()
    feats = tok.shape[2]
    squares = jnp.zeros((rows, LANES), F32)
    for b in range(n_tp):
        x = tok[b].astype(F32)
        for l in range(feats // LANES):
            y = x[:, l * LANES:(l + 1) * LANES]
            squares = squares + y * y
    inverse = lax.rsqrt(jnp.sum(squares, axis=1, keepdims=True) / (n_tp * feats) + EPS)
    for b in range(n_tp):
        cols = slice(b * feats, (b + 1) * feats)
        normed[:, cols] = (tok[b].astype(F32) * inverse * gain[:, cols]).astype(BF16)
    relay_step(nz - 1)
    loads[8].wait()
    val_t[...] = dot(normed[...], wval[...]).T.astype(BF16)
    drift_col = jnp.broadcast_to(drift[z], (LANES, rows)).T
    tri = (lax.broadcasted_iota(jnp.int32, (rows, rows), 1)
           > lax.broadcasted_iota(jnp.int32, (rows, rows), 0)).astype(BF16)

    own = s * nz + z

    def part_to(zo, sd):
        return remote(part_send.at[zo, pl.ds(pl.multiple_of(sd * vals, vals), vals), :], part_recv.at[own],
                      part_s.at[zo, sd], part_r.at[own], sd, zo * PAIR + c)

    def tot_to(zo, sd):
        return remote(tot_send.at[zo], tot_recv.at[own], tot_s.at[zo, sd], tot_r.at[own],
                      sd, zo * PAIR + c)

    for i in range(1, nz):
        zo = (z + i) % nz
        pltpu.make_async_copy(biases.at[zo], biases.at[zo], bias_r.at[zo]).wait()

    def nearest(j):
        low = z < nz // 2
        edge = jnp.where(low, z, nz - 1 - z)
        at = jnp.where(j == 0, edge, jnp.where(j - 1 < edge, j - 1, j))
        return jnp.where(low, at, nz - 1 - at)

    def block(j, carry):
        zo = nearest(j)

        @pl.when(j > 0)
        def _():
            pltpu.make_async_copy(w_slot(zo, corner), w_slot(zo, corner), w_r.at[zo, corner]).wait()
        proj = dot(normed[...], wbuf[zo])
        key = proj[:, :LANES].astype(BF16).astype(F32)
        gate = proj[:, LANES:].astype(BF16).astype(F32)
        u = gate + biases[zo] + drift_col
        log_decay = (jnp.minimum(u, 0.0) - jnp.log1p(jnp.exp(-jnp.abs(u)))) / GATE_NORM
        high = log_decay.astype(BF16)
        low = (log_decay - high.astype(F32)).astype(BF16)
        later = dot(tri, jnp.concatenate([high, low], axis=1))
        rest = later[:, :LANES] + later[:, LANES:]
        weighted = (key * jnp.exp(rest)).astype(BF16)
        tot_send[zo] = jnp.sum(log_decay, axis=0, keepdims=True)
        part_send[zo] = dot(val_t[...], weighted).astype(BF16)
        for i in range(1, n_sp):
            sd = (s + i) % n_sp
            part_to(zo, sd).start()
            tot_to(zo, sd).start()

        @pl.when(j > 0)
        def _():
            part_to(zo, s).start()
            tot_to(zo, s).start()
        return carry
    lax.fori_loop(0, nz, block, 0)
    part_recv[own] = part_send[z, pl.ds(pl.multiple_of(s * vals, vals), vals), :]
    tot_recv[own] = tot_send[z]

    def arrived(d, carry):
        src = (own + d) % (n_sp * nz)
        pltpu.make_async_copy(part_recv.at[src], part_recv.at[src], part_r.at[src]).wait()
        pltpu.make_async_copy(tot_recv.at[src], tot_recv.at[src], tot_r.at[src]).wait()
        return carry
    lax.fori_loop(1, n_sp * nz, arrived, 0)

    later = jnp.zeros((1, LANES), F32)
    total = jnp.zeros((vals, LANES), F32)
    for k in reversed(range(n_sp * nz)):
        total = total + jnp.exp(later) * part_recv[k].astype(F32)
        later = later + tot_recv[k]
    scaled = query[...].astype(F32) * query_scale
    rd_send[...] = jnp.sum((total * scaled).T, axis=0, keepdims=True)
    rd_recv[me] = rd_send[...]

    def read_to(d):
        other = (me + d) % n
        return remote(rd_send, rd_recv.at[me], rd_s.at[d], rd_r.at[me], other // n_tp, other % n_tp)

    def send_read(d, carry):
        read_to(d).start()
        return carry
    lax.fori_loop(1, n, send_read, 0)
    state_out[...] = total.T.astype(BF16)

    for dz in (1, -1):
        for k in range(nz - 1):
            zo = z - k * dz

            @pl.when((zo >= 0) & (zo < nz) & (z + dz >= 0) & (z + dz < nz))
            def _():
                along(zo, dz, k).wait_send()
    for i in range(1, nz):
        to_column(i).wait_send()
        bias_to(i).wait_send()
        for j in range(2):
            in_plane((z + i) % nz, j).wait_send()
            relay((z + i) % nz, j).wait_send()
    for zo in range(nz):
        to_pair(zo).wait_send()

    def sent(j, carry):
        zo = nearest(j)
        for i in range(1, n_sp):
            sd = (s + i) % n_sp
            part_to(zo, sd).wait_send()
            tot_to(zo, sd).wait_send()

        @pl.when(j > 0)
        def _():
            part_to(zo, s).wait_send()
            tot_to(zo, s).wait_send()
        return carry
    lax.fori_loop(0, nz, sent, 0)

    def read_from(d, carry):
        src = (me + d) % n
        pltpu.make_async_copy(rd_recv.at[src], rd_recv.at[src], rd_r.at[src]).wait()
        return carry
    lax.fori_loop(1, n, read_from, 0)

    def read_sent(d, carry):
        read_to(d).wait_send()
        return carry
    lax.fori_loop(1, n, read_sent, 0)

    heads = read_out.shape[0]
    per_head = n_tp // heads

    def head_row(sp, h):
        row = rd_recv[sp * n_tp + h * per_head]
        for i in range(1, per_head):
            row = row + rd_recv[sp * n_tp + h * per_head + i]
        return row
    for h in range(heads):
        squared = jnp.zeros((1, LANES), F32)
        for sp in range(n_sp):
            row = head_row(sp, h)
            squared = squared + row * row
        mean = jnp.sum(squared, axis=1, keepdims=True) / (n_sp * vals)
        read_out[h:h + 1, :] = head_row(s, h) * lax.rsqrt(mean + EPS) * out_gain[h:h + 1, :]


def fused_body(tokens, norm_gain, w_key, w_decay, w_value, decay_bias, gate_drift, queries, out_gain):
    n_sp, n_tp = lax.axis_size("sp"), lax.axis_size("tp")
    nz = n_tp // PAIR
    span, feats = tokens.shape
    width = feats * n_tp
    rows = span // nz
    channels = w_key.shape[1]
    vals = out_gain.shape[1]
    values = w_value.shape[1]
    vmem = pl.BlockSpec(memory_space=pltpu.VMEM)
    hbm = pl.BlockSpec(memory_space=pltpu.HBM)
    dma = pltpu.SemaphoreType.DMA
    return pl.pallas_call(
        functools.partial(kernel, n_sp, n_tp, KEY_CHANNELS ** (-0.5)),
        out_shape=(jax.ShapeDtypeStruct((channels, vals), BF16),
                   jax.ShapeDtypeStruct(out_gain.shape, F32)),
        in_specs=[hbm] * 9,
        out_specs=(vmem, vmem),
        scratch_shapes=[
            pltpu.VMEM(tokens.shape, BF16),
            pltpu.VMEM((1, width), F32),
            pltpu.VMEM((nz, 1, rows), F32),
            pltpu.VMEM((1, channels), BF16),
            pltpu.VMEM(out_gain.shape, F32),
            pltpu.VMEM((n_tp, rows, feats), BF16),
            pltpu.VMEM((nz, width, 2 * channels), BF16),
            pltpu.VMEM((width, values), BF16),
            pltpu.VMEM((rows, width), BF16),
            pltpu.VMEM((values, rows), BF16),
            pltpu.VMEM((nz, 1, channels), F32),
            pltpu.VMEM((nz, values, channels), BF16),
            pltpu.VMEM((n_sp * nz, vals, channels), BF16),
            pltpu.VMEM((nz, 1, channels), F32),
            pltpu.VMEM((n_sp * nz, 1, channels), F32),
            pltpu.VMEM((1, vals), F32),
            pltpu.VMEM((n_sp * n_tp, 1, vals), F32),
            dma((9,)),
            dma((nz - 1,)), dma((n_tp,)),
            dma((nz,)), dma((nz,)),
            dma((2, nz)), dma((nz, n_sp)), dma((nz, 4)),
            dma((nz - 1,)), dma((nz,)),
            dma((nz, n_sp)), dma((n_sp * nz,)),
            dma((nz, n_sp)), dma((n_sp * nz,)),
            dma((n_sp * n_tp,)), dma((n_sp * n_tp,)),
        ],
        compiler_params=pltpu.CompilerParams(
            collective_id=0, has_side_effects=True, vmem_limit_bytes=VMEM_BYTES),
    )(tokens, norm_gain.reshape(1, width), w_key, w_decay, w_value, decay_bias.reshape(1, channels),
      gate_drift.reshape(nz, 1, rows), queries.reshape(1, channels), out_gain)


def fits(tokens, w_key, w_value, out_gain, n_tp):
    nz = n_tp // PAIR
    return (lax.axis_size("sp") == PLANE and n_tp % PAIR == 0 and nz > 1 and tokens.shape[0] % (nz * LANES) == 0
            and tokens.shape[1] % LANES == 0 and w_key.shape[1] == LANES and out_gain.shape[1] == LANES
            and n_tp % out_gain.shape[0] == 0)


def choose(tokens, norm_gain, w_key, w_decay, w_value, decay_bias, gate_drift, queries, out_gain):
    args = (tokens, norm_gain, w_key, w_decay, w_value, decay_bias, gate_drift, queries, out_gain)
    if fits(tokens, w_key, w_value, out_gain, lax.axis_size("tp")):
        return fused_body(*args)
    return body(*args)


def solution(mesh):
    return jax.shard_map(
        choose,
        mesh=mesh,
        in_specs=(
            P("sp", "tp"),
            P(),
            P(None, "tp"),
            P(None, "tp"),
            P(),
            P("tp"),
            P("sp"),
            P("tp"),
            P(None, "sp"),
        ),
        out_specs=(P("tp", "sp"), P(None, "sp")),
        check_vma=False,
    )
```
